32 devices in a mesh: ep: 8 (over z, x), tp: 4 (over y, core).
Axes of the slice: x: 2, y: 2, z: 4, core: 2. Of those that a mesh axis runs over, the one named last changes fastest.
Arguments:
- query_logits: bfloat16 [2048, 2048], P('ep', 'tp'), may hold values from -6 to 6
- forget_gate_logits: bfloat16 [2048, 2048], P('ep', 'tp'), may hold values from -3.75 to 3.75
- written_values: bfloat16 [2048, 2048], P('ep', 'tp'), may hold values from -6 to 6
- output_gate_logits: bfloat16 [2048, 2048], P('ep', 'tp'), may hold values from -6 to 6
- gap: float32 [2048], P('tp'), may hold values from 4.8828125e-05 to 0.06
- extra_log_forget: float32 [2048, 2048], P('ep', 'tp'), may hold values from -0.7 to 0
- head_norm_scale: float32 [2048], P('tp'), may hold values from 0.1 to 1.9
- mixer_output_matrix: bfloat16 [2048, 2048], P('tp'), may hold values from -0.125 to 0.125
- expert_input_tokens: bfloat16 [2048, 2048], P('ep'), may hold values from -12 to 12
- expert_norm_scale: float32 [2048], replicated, may hold values from 0.1 to 1.9
- routes: int32 [2048, 2], P('ep'), may hold values from 0 to 7, all different within a row; in each aligned block of 256 rows (0 to 255, 256 to 511, ...) at most 96 rows name the same one
- router_scores_chosen: float32 [2048, 2], P('ep'), may hold values from -6 to 6
- expert_gate_matrix: bfloat16 [8, 2048, 4096], P('ep', None, 'tp'), may hold values from -0.125 to 0.125
- expert_up_matrix: bfloat16 [8, 2048, 4096], P('ep', None, 'tp'), may hold values from -0.125 to 0.125
- expert_down_matrix: bfloat16 [8, 2048, 4096], P('ep', None, 'tp'), may hold values from -0.09375 to 0.09375
Outputs:
- mixer_output_rows: bfloat16 [2048, 2048], P(('ep', 'tp'))
- expert_out: bfloat16 [2048, 2048], P('ep', 'tp')
The draws below stay inside these ranges and needn't reach their ends.
Inputs may be any that keep to these rules, and one draw needn't show every extreme that they name: `routes`: each row names two different experts. Among the rows of one device no expert is named more than 96 times, and 96 is reached in some blocks.
All inputs are finite; a program needn't handle non-finite values.
Results may differ from the reference program's by a relative error of at most 0.019.
Values may be sent and summed in bfloat16 or wider, within the bound.
A program may use at most 64 MiB of HBM per device.

```python
import math
import jax
import jax.numpy as jnp
import numpy as np
from jax import lax

HEAD_DIM = 128
HEADS = 16
D = 2048
FF = 4096
TOK_A = 256
TOK_B = 256
TOKENS_A = 2048
TOKENS_B = 2048
EXPERTS = 8
CAP = 96
N_EP = 8
N_TP = 4


def draw_gap(key, part):
    choose_key, lasting_key, quick_key = jax.random.split(jax.random.fold_in(key, 11), 3)
    quick_heads = jax.random.uniform(choose_key, (HEADS,)) < 0.5
    lasting = jnp.exp(jax.random.uniform(lasting_key, (HEADS, HEAD_DIM), jnp.float32, math.log(0.1 / TOKENS_A), math.log(1.0 / TOKENS_A)))
    quick = jnp.exp(jax.random.uniform(quick_key, (HEADS, HEAD_DIM), jnp.float32, math.log(0.02), math.log(0.06)))
    return jnp.where(quick_heads[:, None], quick, lasting).reshape(D).astype(jnp.float32)


def draw_forget_gate_logits(key, part):
    noise_key, shift_key = jax.random.split(jax.random.fold_in(key, 23), 2)
    block_shift = jax.random.uniform(shift_key, (N_EP,), jnp.float32, -1.2, 1.2)
    noise = jnp.clip(jax.random.normal(noise_key, (TOKENS_A, D), jnp.float32), -2.5, 2.5)
    return (noise + jnp.repeat(block_shift, TOK_A)[:, None]).astype(jnp.bfloat16)


def draw_extra_log_forget(key, part):
    where_key, depth_key = jax.random.split(jax.random.fold_in(key, 37), 2)
    spots = jax.random.randint(where_key, (3,), 0, TOKENS_A)
    struck = jnp.any(jnp.arange(TOKENS_A)[:, None] == spots[None, :], axis=1)
    depth = jnp.log(jax.random.uniform(depth_key, (TOKENS_A, D), jnp.float32, 0.5, 0.8))
    return jnp.where(struck[:, None], depth, 0.0).astype(jnp.float32)


def draw_expert_input_tokens(key, part):
    noise_key, scale_key = jax.random.split(jax.random.fold_in(key, 41), 2)
    scales = jnp.exp(jax.random.uniform(scale_key, (TOKENS_B, 1), jnp.float32, math.log(0.3), math.log(3.0)))
    noise = jnp.clip(jax.random.normal(noise_key, (TOKENS_B, D), jnp.float32), -4.0, 4.0)
    return (noise * scales).astype(jnp.bfloat16)


def block_levels(rng, dims, pieces, least, high):
    gain, own = 1.0, jax.random.fold_in(rng, 6)
    for dim, parts in pieces:
        steps = jnp.exp(jax.random.uniform(jax.random.fold_in(own, dim), (parts,), jnp.float32, least / len(pieces), high / len(pieces)))
        gain = gain * jnp.repeat(steps, dims[dim] // parts).reshape([-1 if axis == dim else 1 for axis in range(len(dims))])
    return gain


def deal_out(rng, own, number, rows, amount, top, most, skew):
    ranking = jax.random.permutation(rng, amount)
    crowded, ordinary = shares(amount, rows * top, most, skew, True), shares(amount, rows * top, most, skew, False)
    places = jnp.arange(amount)

    def named(sizes, offset_by):
        used = int((sizes > 0).sum())
        fixed = max(1, used // 4)
        passed = fixed + (places - fixed + offset_by * (used - fixed)) % max(1, amount - fixed)
        return jnp.zeros((amount,), jnp.int32).at[ranking[jnp.where(places < fixed, places, passed)]].set(jnp.asarray(sizes, jnp.int32))

    sizes = jnp.where(number % 4 == 0, named(crowded, number // 4), named(ordinary, number - number // 4 - 1))
    mixed = jax.random.permutation(jax.random.fold_in(own, 3), amount)
    source_of, taker = mixed[0:amount // 2 * 2:2], mixed[1:amount // 2 * 2:2]
    room = jnp.minimum(sizes[source_of] - 1, most - sizes[taker]) // 2
    room = jnp.where((source_of == ranking[0]) | (taker == ranking[0]) | (sizes[taker] == 0), 0, jnp.maximum(room, 0))
    passed = jax.random.randint(jax.random.fold_in(own, 4), (amount // 2,), 0, 1 << 20) % (room + 1)
    sizes = sizes.at[source_of].add(-passed).at[taker].add(passed)
    members = jnp.searchsorted(jnp.cumsum(sizes), jnp.arange(rows * top), side="right").astype(jnp.int32)
    table = members.reshape(top, rows).T
    table = table[jax.random.permutation(jax.random.fold_in(own, 1), rows)]
    offset_by = jax.random.randint(jax.random.fold_in(own, 2), (rows, 1), 0, top)
    return jnp.take_along_axis(table, (jnp.arange(top)[None, :] + offset_by) % top, axis=1)


def shares(number_of, total, limit, skew, full):
    portions = [(1 << 20) // math.isqrt(standing ** skew) + 1 for standing in range(1, number_of + 1)]
    largest = limit if full else min(limit, max(-(-total // number_of), total * portions[0] // sum(portions)))
    least = 1 if total - largest >= number_of - 1 else 0
    counts, spare = [largest] + [least] * (number_of - 1), total - largest - least * (number_of - 1)
    while spare > 0:
        free = [i for i in range(1, number_of) if counts[i] < largest] or [i for i in range(1, number_of) if counts[i] < limit]
        mass, left = sum([portions[i] for i in free]), spare
        for i in free:
            extra = min(limit - counts[i], max(1, left * portions[i] // mass), spare)
            counts[i] = counts[i] + extra
            spare = spare - extra
    return np.array(counts)


def gaussian(stream_key, shape, deviation, limit, shards=(), kind=jnp.bfloat16):
    loudness = block_levels(stream_key, shape, shards, -0.22, 0.18) if shards else 1.0
    drawn = jax.random.normal(stream_key, shape, jnp.float32) * deviation * loudness
    return jnp.minimum(jnp.maximum(drawn, -limit), limit).astype(kind)


def setup_inputs(seed: int = 0) -> dict:
    streams_of = jax.random.split(jax.random.key(seed), 16)
    query_logits = gaussian(streams_of[0], (TOKENS_A, D), 1.0, 6.0, ((0, 8), (1, 4)))
    forget_gate_logits = draw_forget_gate_logits(jax.random.fold_in(streams_of[15], 71), 0)
    written_values = gaussian(streams_of[2], (TOKENS_A, D), 1.0, 6.0, ((0, 8), (1, 4)))
    output_gate_logits = gaussian(streams_of[3], (TOKENS_A, D), 1.0, 6.0, ((0, 8), (1, 4)))
    gap = draw_gap(jax.random.fold_in(streams_of[15], 71), 0)
    extra_log_forget = draw_extra_log_forget(jax.random.fold_in(streams_of[15], 71), 0)
    head_norm_scale = jnp.clip(1.0 + 0.18 * jax.random.normal(streams_of[6], (D,), jnp.float32), 0.1, 1.9)
    mixer_output_matrix = gaussian(streams_of[7], (D, D), D ** -0.5, 0.125, ((0, 4),))
    expert_input_tokens = draw_expert_input_tokens(jax.random.fold_in(streams_of[15], 71), 0)
    expert_norm_scale = jnp.clip(1.0 + 0.18 * jax.random.normal(streams_of[9], (D,), jnp.float32), 0.1, 1.9)
    routes_keys = jax.random.split(jax.random.fold_in(streams_of[10], 1), TOKENS_B // TOK_B)
    routes_turns = jax.random.permutation(jax.random.fold_in(streams_of[10], 3), TOKENS_B // TOK_B)
    routes = jax.vmap(lambda own, number: deal_out(jax.random.fold_in(streams_of[10], 2), own, number, TOK_B, EXPERTS, 2, CAP, 2))(routes_keys, routes_turns).reshape((TOKENS_B, 2))
    router_scores_chosen = gaussian(streams_of[11], (TOKENS_B, 2), 1.5, 6.0, ((0, 8),), jnp.float32)
    expert_gate_matrix = gaussian(streams_of[12], (EXPERTS, D, FF), D ** -0.5, 0.125, ((0, 8), (2, 4)))
    expert_up_matrix = gaussian(streams_of[13], (EXPERTS, D, FF), D ** -0.5, 0.125, ((0, 8), (2, 4)))
    expert_down_matrix = gaussian(streams_of[14], (EXPERTS, D, FF), FF ** -0.5, 0.09375, ((0, 8), (2, 4)))
    return {"query_logits": query_logits, "forget_gate_logits": forget_gate_logits, "written_values": written_values, "output_gate_logits": output_gate_logits, "gap": gap, "extra_log_forget": extra_log_forget, "head_norm_scale": head_norm_scale, "mixer_output_matrix": mixer_output_matrix, "expert_input_tokens": expert_input_tokens, "expert_norm_scale": expert_norm_scale, "routes": routes, "router_scores_chosen": router_scores_chosen, "expert_gate_matrix": expert_gate_matrix, "expert_up_matrix": expert_up_matrix, "expert_down_matrix": expert_down_matrix}


exact_precision = lax.Precision.HIGHEST

def recurrent_portion(query_logits, forget_gate_logits, written_values, output_gate_logits, gap, extra_log_forget, head_norm_scale, mixer_output_matrix):
    final_result = gap * jax.nn.sigmoid(-forget_gate_logits.astype(jnp.float32))
    decay_logarithm = jnp.log1p(-final_result) + extra_log_forget
    queries = jax.nn.silu(query_logits.astype(jnp.float32))
    values = written_values.astype(jnp.float32)

    def by_head(array):
        return array.reshape(TOKENS_A, HEADS, HEAD_DIM)

    def advance(state, inputs):
        query_now, key_now, value_now, decay_now = inputs
        state = jnp.exp(decay_now)[:, :, None] * state + key_now[:, :, None] * value_now[:, None, :]
        output = jnp.einsum('hd,hdv->hv', query_now, state, precision=exact_precision)
        return (state, output)
    start_state = jnp.zeros((HEADS, HEAD_DIM, HEAD_DIM), jnp.float32)
    _, recurrent = lax.scan(advance, start_state, (by_head(queries), by_head(final_result), by_head(values), by_head(decay_logarithm)))
    scaled = recurrent * lax.rsqrt(lax.optimization_barrier(jnp.mean(recurrent * recurrent, axis=-1, keepdims=True)) + 1e-06)
    scaled = scaled.reshape(TOKENS_A, D)
    hidden = (scaled * head_norm_scale * jax.nn.silu(output_gate_logits.astype(jnp.float32))).astype(jnp.bfloat16)
    group_width = D // N_TP

    def add_group(totals, index):
        columns = lax.dynamic_slice_in_dim(hidden, index * group_width, group_width, 1)
        weight_rows = lax.dynamic_slice_in_dim(mixer_output_matrix, index * group_width, group_width, 0)
        partial_sum = jnp.dot(columns, weight_rows, preferred_element_type=jnp.float32)
        rounded = lax.optimization_barrier(partial_sum.astype(jnp.bfloat16)).astype(jnp.float32)
        return (totals + rounded, None)
    mixed_total, _ = lax.scan(add_group, jnp.zeros((TOKENS_A, D), jnp.float32), jnp.arange(N_TP, dtype=jnp.int32))
    return mixed_total.astype(jnp.bfloat16)

def expert_part(expert_input_tokens, expert_norm_scale, routes, router_scores_chosen, expert_gate_matrix, expert_up_matrix, expert_down_matrix):
    inputs32 = expert_input_tokens.astype(jnp.float32)
    centred = inputs32 - lax.optimization_barrier(jnp.mean(inputs32, axis=-1, keepdims=True))
    variance = lax.optimization_barrier(jnp.mean(centred * centred, axis=-1, keepdims=True))
    normed = (centred * lax.rsqrt(variance + 1e-05) * expert_norm_scale).astype(jnp.bfloat16)
    first_weight = jax.nn.sigmoid(router_scores_chosen[:, 0] - router_scores_chosen[:, 1])
    route_weight = jnp.stack([first_weight, 1.0 - first_weight], axis=1)
    flat_routes = routes.reshape(N_EP, TOK_B * 2)
    onehot = (flat_routes[:, :, None] == jnp.arange(EXPERTS, dtype=jnp.int32)[None, None, :]).astype(jnp.int32)
    earlier = jnp.cumsum(onehot, axis=1) - onehot
    position = lax.optimization_barrier(jnp.sum(earlier * onehot, axis=2))
    slot_count = N_EP * CAP
    source = jnp.arange(N_EP, dtype=jnp.int32)[:, None]
    target = (flat_routes * slot_count + source * CAP + position).reshape(-1).astype(jnp.int32)
    token_ids = jnp.arange(TOKENS_B * 2, dtype=jnp.int32) // 2
    owner = jnp.zeros((EXPERTS * slot_count,), jnp.int32).at[target].set(token_ids)
    filled = jnp.zeros((EXPERTS * slot_count,), jnp.bool_).at[target].set(True)
    group_width = FF // N_TP

    def one_expert(unused, inputs):
        owner_ids, live_slots, gate_w, up_w, down_w = inputs
        picked = jnp.where(live_slots[:, None], normed[owner_ids], jnp.zeros((), jnp.bfloat16))
        gate_act = jnp.dot(picked, gate_w, preferred_element_type=jnp.float32)
        up_act = jnp.dot(picked, up_w, preferred_element_type=jnp.float32)
        hidden = (jax.nn.silu(gate_act) * up_act).astype(jnp.bfloat16)

        def add_group(totals, index):
            hidden_cols = lax.dynamic_slice_in_dim(hidden, index * group_width, group_width, 1)
            down_cols = lax.dynamic_slice_in_dim(down_w, index * group_width, group_width, 1)
            partial_sum = lax.dot_general(hidden_cols, down_cols, (((1,), (1,)), ((), ())), preferred_element_type=jnp.float32)
            rounded = lax.optimization_barrier(partial_sum.astype(jnp.bfloat16)).astype(jnp.float32)
            return (totals + rounded, None)
        summed, _ = lax.scan(add_group, jnp.zeros((slot_count, D), jnp.float32), jnp.arange(N_TP, dtype=jnp.int32))
        return (unused, summed.astype(jnp.bfloat16))
    _, results = lax.scan(one_expert, None, (owner.reshape(EXPERTS, slot_count), filled.reshape(EXPERTS, slot_count), expert_gate_matrix, expert_up_matrix, expert_down_matrix))
    chosen = results.reshape(EXPERTS * slot_count, D)[target].astype(jnp.float32).reshape(TOKENS_B, 2, D)
    return lax.optimization_barrier(jnp.sum(chosen * route_weight[:, :, None], axis=1)).astype(jnp.bfloat16)

def reference(query_logits, forget_gate_logits, written_values, output_gate_logits, gap, extra_log_forget, head_norm_scale, mixer_output_matrix, expert_input_tokens, expert_norm_scale, routes, router_scores_chosen, expert_gate_matrix, expert_up_matrix, expert_down_matrix):
    mixer_output_rows = recurrent_portion(query_logits, forget_gate_logits, written_values, output_gate_logits, gap, extra_log_forget, head_norm_scale, mixer_output_matrix)
    expert_out = expert_part(expert_input_tokens, expert_norm_scale, routes, router_scores_chosen, expert_gate_matrix, expert_up_matrix, expert_down_matrix)
    return (mixer_output_rows, expert_out)
```

```python
import functools

import jax
import jax.numpy as jnp
from jax import lax
from jax.experimental import pallas as pl
from jax.experimental.pallas import tpu as pltpu
from jax.sharding import PartitionSpec as P

HEAD_DIM = 128
CHUNK = 64
MESH = pl.DeviceIdType.MESH
F32 = jnp.float32
BF16 = jnp.bfloat16


def flip(i, k):
    b = 1
    while b <= k:
        if k & b:
            i = i + b - 2 * b * lax.rem(lax.div(i, b), 2)
        b *= 2
    return i


def kernel(
    E, T, cap, pieces,
    q_ref, f_ref, v_ref, o_ref, gap_ref, extra_ref, hscale_ref,
    mixw_hbm, tok_ref, escale_ref, routes_ref, scores_ref,
    gate_hbm, up_hbm, down_hbm,
    mix_out, exp_out,
    gate, up, down, mixw,
    ncols, dmat, wmat, outgoing, feats, hidden, part, precv, xsend, xrecv, fin, ret,
    qs, ks, run, qg, rec, ist, idec, est, edec, ksend, krecv,
    mhid, mpart, mprecv, mxsend, mxrecv,
    wsem, send_sem, recv_sem,
):
    me = lax.axis_index("ep")
    t = lax.axis_index("tp")
    G = T // 2
    g, c = lax.div(t, 2), lax.rem(t, 2)
    oc = 1 - c
    tokens, width = q_ref.shape
    heads = width // HEAD_DIM
    S = E * cap
    Dl = ncols.shape[1]
    FFl = hidden.shape[1]

    loads = [
        pltpu.make_async_copy(src, dst, wsem.at[i])
        for i, (src, dst) in enumerate(
            ((gate_hbm, gate), (up_hbm, up), (down_hbm, down), (mixw_hbm, mixw))
        )
    ]
    for load in loads:
        load.start()

    barrier = pltpu.get_barrier_semaphore()
    for k in range(1, E):
        pl.semaphore_signal(barrier, inc=1, device_id=(flip(me, k), t), device_id_type=MESH)
    pl.semaphore_signal(barrier, inc=1, device_id=(me, 2 * g + oc), device_id_type=MESH)
    for j in range(1, G):
        pl.semaphore_signal(
            barrier, inc=1, device_id=(me, 2 * flip(g, j) + c), device_id_type=MESH
        )

    used = [0]

    def remote(src, dst, device):
        slot = used[0]
        used[0] += 1
        return pltpu.make_async_remote_copy(
            src_ref=src, dst_ref=dst, send_sem=send_sem.at[slot], recv_sem=recv_sem.at[slot],
            device_id=device, device_id_type=MESH,
        )

    def arrival(src, dst, copy_slot):
        return pltpu.make_async_remote_copy(
            src_ref=src, dst_ref=dst, send_sem=send_sem.at[copy_slot],
            recv_sem=recv_sem.at[copy_slot], device_id=(me, t), device_id_type=MESH,
        )

    sent = []

    x = tok_ref[...].astype(F32)
    mean = jnp.mean(x, axis=-1, keepdims=True)
    centred = x - mean
    inv = lax.rsqrt(jnp.mean(centred * centred, axis=-1, keepdims=True) + 1e-05)
    cols = pl.ds(pl.multiple_of(t * Dl, 128), Dl)
    ncols[...] = ((tok_ref[:, cols].astype(F32) - mean) * inv * escale_ref[:, cols]).astype(BF16)

    ntok = tok_ref.shape[0]
    ek = lax.broadcasted_iota(jnp.int32, (E, ntok), 0) ^ me
    first, second = routes_ref[0:1, :] == ek, routes_ref[1:2, :] == ek
    named = jnp.where(first | second, 1.0, 0.0)
    earlier = jnp.where(
        lax.broadcasted_iota(jnp.int32, (ntok, ntok), 0)
        < lax.broadcasted_iota(jnp.int32, (ntok, ntok), 1), 1.0, 0.0
    ).astype(BF16)
    position = jnp.dot(named.astype(BF16), earlier, preferred_element_type=F32)
    place = jnp.where(first | second, position, -1.0).astype(jnp.int32)
    w0 = jax.nn.sigmoid(scores_ref[0:1, :] - scores_ref[1:2, :])
    weight = jnp.where(first, w0, jnp.where(second, 1.0 - w0, 0.0))
    rows = lax.broadcasted_iota(jnp.int32, (cap, ntok), 0)
    for k in range(E):
        hit = rows == place[k:k + 1, :]
        dmat[k * cap:(k + 1) * cap, :] = jnp.where(hit, 1.0, 0.0).astype(BF16)
        wmat[k * cap:(k + 1) * cap, :] = jnp.where(hit, weight[k:k + 1, :], 0.0).astype(BF16)
    outgoing[...] = jnp.dot(dmat[...], ncols[...], preferred_element_type=F32).astype(BF16)
    feats[t, 0:cap, :] = outgoing[0:cap, :]

    pl.semaphore_wait(barrier, E - 1 + 1 + G - 1)

    dispatch = {}
    for k in range(1, E):
        block = pl.ds(k * cap, cap)
        dispatch[k] = remote(outgoing.at[block], feats.at[t, block], (flip(me, k), t))
        dispatch[k].start()
        sent.append(dispatch[k])

    closing = gap_ref[...] * jax.nn.sigmoid(-f_ref[...].astype(F32))
    ks[...] = closing
    logd = jnp.log1p(-closing) + extra_ref[...]
    qs[...] = jax.nn.silu(q_ref[...].astype(F32))
    r_i = lax.broadcasted_iota(jnp.int32, (CHUNK, CHUNK), 0)
    c_i = lax.broadcasted_iota(jnp.int32, (CHUNK, CHUNK), 1)
    causal = r_i >= c_i
    tri = jnp.where(causal, 1.0, 0.0).astype(F32)
    nchunks = tokens // CHUNK
    for n in range(nchunks):
        run[n * CHUNK:(n + 1) * CHUNK, :] = jnp.dot(
            tri, logd[n * CHUNK:(n + 1) * CHUNK, :], precision=lax.Precision.HIGHEST,
            preferred_element_type=F32,
        )

    def head_local(h, _):
        lanes = pl.ds(pl.multiple_of(h * HEAD_DIM, HEAD_DIM), HEAD_DIM)
        state = jnp.zeros((HEAD_DIM, HEAD_DIM), F32)
        before = jnp.zeros((1, HEAD_DIM), F32)
        for n in range(nchunks):
            rs = slice(n * CHUNK, (n + 1) * CHUNK)
            r = run[rs, lanes]
            total = r[CHUNK - 1:CHUNK, :]
            qd = qs[rs, lanes] * jnp.exp(r)
            key = ks[rs, lanes]
            kd = (key * jnp.exp(-r)).astype(BF16)
            kst = (key * jnp.exp(total - r)).astype(BF16)
            val = v_ref[rs, lanes]
            qd_b = qd.astype(BF16)
            scores = lax.dot_general(
                qd_b, kd, (((1,), (1,)), ((), ())), preferred_element_type=F32
            )
            scores = jnp.where(causal, scores, 0.0).astype(BF16)
            out = jnp.dot(scores, val, preferred_element_type=F32)
            if n:
                out += lax.dot_general(
                    qd_b, state.astype(BF16), (((1,), (1,)), ((), ())),
                    preferred_element_type=F32,
                )
            rec[rs, lanes] = out
            qg[rs, lanes] = (qd * jnp.exp(before)).astype(BF16)
            state = state * jnp.exp(total) + lax.dot_general(
                val, kst, (((0,), (0,)), ((), ())), preferred_element_type=F32
            )
            before = before + total
        ist[h] = state
        idec[h] = jnp.broadcast_to(jnp.exp(before), (16, HEAD_DIM))
        est[h] = jnp.zeros((HEAD_DIM, HEAD_DIM), F32)
        edec[h] = jnp.ones((16, HEAD_DIM), F32)
        return 0

    lax.fori_loop(0, heads, head_local, 0)

    hops = []
    dist = 1
    while dist < E:
        hops.append(dist)
        dist *= 2
    hop_copy = [
        remote(ksend.at[r], krecv.at[r], (lax.rem(me + d, E), t)) for r, d in enumerate(hops)
    ]

    def hop_send(r):
        @pl.when(me + hops[r] < E)
        def _():
            ksend[r, :, 0:HEAD_DIM, :] = ist[...].astype(BF16)
            ksend[r, :, HEAD_DIM:HEAD_DIM + 16, :] = idec[...].astype(BF16)
            hop_copy[r].start()

    def hop_recv(r):
        @pl.when(me >= hops[r])
        def _():
            hop_copy[r].wait_recv()
            s = krecv[r, :, 0:HEAD_DIM, :].astype(F32)
            d = krecv[r, :, HEAD_DIM:HEAD_DIM + 16, :].astype(F32)
            est[...] = edec[:, 0:1, :] * s + est[...]
            edec[...] = edec[...] * d
            if r + 1 < len(hops):
                ist[...] = idec[:, 0:1, :] * s + ist[...]
                idec[...] = idec[...] * d

    hop_send(0)

    ag_partner, ag_cross, rs_partner, rs_cross, back = {}, {}, {}, {}, {}

    def piece_rows(p):
        a, n = pieces[p]
        return pl.ds(a * cap, n * cap)

    def gather_start(p):
        a, n = pieces[p]
        for k in range(max(a, 1), a + n):
            dispatch[k].wait_recv()
        rr = piece_rows(p)
        for j in range(1, G):
            ag_cross[p, j] = remote(feats.at[t, rr], feats.at[t, rr], (me, 2 * flip(g, j) + c))
            ag_cross[p, j].start()
            sent.append(ag_cross[p, j])
        for j in range(G):
            idx = 2 * flip(g, j) + c
            ag_partner[p, j] = (
                used[0], remote(feats.at[idx, rr], feats.at[idx, rr], (me, 2 * g + oc))
            )
        ag_partner[p, 0][1].start()
        sent.append(ag_partner[p, 0][1])

    def gather_relay(p):
        rr = piece_rows(p)
        for j in range(1, G):
            ag_cross[p, j].wait_recv()
            ag_partner[p, j][1].start()
            sent.append(ag_partner[p, j][1])

    def gather_end(p):
        for j in range(G):
            ag_partner[p, j][1].wait_recv()

    tile = min(256, FFl)

    def experts(p):
        a, n = pieces[p]
        rs = slice(a * cap, (a + n) * cap)

        def one(i, _):
            cc = pl.ds(pl.multiple_of(i * tile, tile), tile)
            ga = jnp.zeros((n * cap, tile), F32)
            ua = jnp.zeros((n * cap, tile), F32)
            for d in range(T):
                xs = feats[d, rs, :]
                ga += jnp.dot(xs, gate[d * Dl:(d + 1) * Dl, cc], preferred_element_type=F32)
                ua += jnp.dot(xs, up[d * Dl:(d + 1) * Dl, cc], preferred_element_type=F32)
            hidden[rs, cc] = (jax.nn.silu(ga) * ua).astype(BF16)
            return 0

        lax.fori_loop(0, FFl // tile, one, 0)

        def down_group(cls, gg):
            ff = pl.ds(pl.multiple_of((2 * gg + cls) * Dl, 128), Dl)
            part[cls, gg, rs, :] = lax.dot_general(
                hidden[rs, :], down[ff, :], (((1,), (1,)), ((), ())),
                preferred_element_type=F32,
            ).astype(BF16)

        def theirs(gg, _):
            down_group(oc, gg)
            return 0

        def ours(gg, _):
            down_group(c, gg)
            return 0

        lax.fori_loop(0, G, theirs, 0)
        rr = piece_rows(p)
        rs_partner[p] = remote(part.at[oc, :, rr], precv.at[:, rr], (me, 2 * g + oc))
        rs_partner[p].start()
        sent.append(rs_partner[p])
        lax.fori_loop(0, G, ours, 0)

    def scatter_cross(p):
        a, n = pieces[p]
        rs = slice(a * cap, (a + n) * cap)
        rr = piece_rows(p)
        rs_partner[p].wait_recv()
        for j in range(1, G):
            gj = flip(g, j)
            xsend[j - 1, rs, :] = (
                part[c, gj, rs, :].astype(F32) + precv[gj, rs, :].astype(F32)
            ).astype(BF16)
            rs_cross[p, j] = remote(
                xsend.at[j - 1, rr], xrecv.at[j - 1, rr], (me, 2 * gj + c)
            )
            rs_cross[p, j].start()
            sent.append(rs_cross[p, j])

    def give_back(p):
        a, n = pieces[p]
        rs = slice(a * cap, (a + n) * cap)
        total = part[c, g, rs, :].astype(F32) + precv[g, rs, :].astype(F32)
        for j in range(1, G):
            rs_cross[p, j].wait_recv()
            total += xrecv[j - 1, rs, :].astype(F32)
        fin[rs, :] = total.astype(BF16)
        for k in range(max(a, 1), a + n):
            block = pl.ds(k * cap, cap)
            back[k] = remote(fin.at[block], ret.at[block], (flip(me, k), t))
            back[k].start()
            sent.append(back[k])
        if a == 0:
            ret[0:cap, :] = fin[0:cap, :]

    def mixer_end():
        for load in loads[3:]:
            load.wait()
        for h in range(heads):
            lanes = slice(h * HEAD_DIM, (h + 1) * HEAD_DIM)
            r = rec[:, lanes] + lax.dot_general(
                qg[:, lanes], est[h].astype(BF16), (((1,), (1,)), ((), ())),
                preferred_element_type=F32,
            )
            r = r * lax.rsqrt(jnp.mean(r * r, axis=-1, keepdims=True) + 1e-06)
            mhid[:, lanes] = (
                r * hscale_ref[:, lanes] * jax.nn.silu(o_ref[:, lanes].astype(F32))
            ).astype(BF16)
        R = mix_out.shape[0]
        wide = mixw.shape[1]
        step = min(512, wide)

        def one(i, _):
            cc = pl.ds(pl.multiple_of(i * step, step), step)
            y = jnp.dot(mhid[...], mixw[:, cc], preferred_element_type=F32).astype(BF16)
            for d in range(T):
                mpart[d % 2, d // 2, :, cc] = y[d * R:(d + 1) * R, :]
            return 0

        lax.fori_loop(0, wide // step, one, 0)
        rs_partner["m"] = remote(mpart.at[oc], mprecv, (me, 2 * g + oc))
        rs_partner["m"].start()
        sent.append(rs_partner["m"])

    def mixer_cross():
        rs_partner["m"].wait_recv()
        for j in range(1, G):
            gj = flip(g, j)
            mxsend[j - 1] = (mpart[c, gj].astype(F32) + mprecv[gj].astype(F32)).astype(BF16)
            rs_cross["m", j] = remote(mxsend.at[j - 1], mxrecv.at[j - 1], (me, 2 * gj + c))
            rs_cross["m", j].start()
            sent.append(rs_cross["m", j])

    def mixer_out():
        total = mpart[c, g].astype(F32) + mprecv[g].astype(F32)
        for j in range(1, G):
            rs_cross["m", j].wait_recv()
            total += mxrecv[j - 1].astype(F32)
        mix_out[...] = total.astype(BF16)

    last = len(pieces) - 1
    gather_start(0)
    hop_recv(0)
    if len(hops) > 1:
        hop_send(1)
    gather_relay(0)
    for load in loads[:3]:
        load.wait()
    for p in range(len(pieces)):
        if p < last:
            gather_start(p + 1)
        gather_end(p)
        if p == 0:
            for r in range(1, len(hops)):
                hop_recv(r)
                if r + 1 < len(hops):
                    hop_send(r + 1)
        if p > 0:
            scatter_cross(p - 1)
        experts(p)
        if p < last:
            gather_relay(p + 1)
        if p > 0:
            give_back(p - 1)
    scatter_cross(last)
    mixer_end()
    give_back(last)
    mixer_cross()
    mixer_out()
    for k in range(1, E):
        back[k].wait_recv()
    exp_out[...] = lax.dot_general(
        wmat[...], ret[...], (((0,), (0,)), ((), ())), preferred_element_type=F32
    ).astype(BF16)
    for copy in sent:
        copy.wait_send()
    for r in range(len(hops)):
        @pl.when(me + hops[r] < E)
        def _():
            hop_copy[r].wait_send()


def body(E, T, q, f, v, o, gap, extra, hscale, mixw, tok, escale, routes, scores, gate, up, down):
    tokens, width = q.shape
    ntok, D = tok.shape
    heads = width // HEAD_DIM
    G = T // 2
    cap = -(-(3 * ntok // E) // 16) * 16
    S = E * cap
    Dl = D // T
    FFl = gate.shape[2]
    R = tokens // T
    half = E // 2
    pieces = ((0, half), (half, half))
    nhops = max(1, (E - 1).bit_length())
    copies = 2 * (E - 1) + nhops + len(pieces) * (G - 1 + G + 1 + G - 1) + G
    vm = pl.BlockSpec(memory_space=pltpu.VMEM)
    anyspace = pl.BlockSpec(memory_space=pl.ANY)
    V = pltpu.VMEM
    scratch = [
        V((D, FFl), BF16), V((D, FFl), BF16), V((D, FFl), BF16), V(mixw.shape, BF16),
        V((ntok, Dl), BF16), V((S, ntok), BF16), V((S, ntok), BF16), V((S, Dl), BF16),
        V((T, S, Dl), BF16), V((S, FFl), BF16), V((2, G, S, Dl), BF16), V((G, S, Dl), BF16),
        V((max(G - 1, 1), S, Dl), BF16), V((max(G - 1, 1), S, Dl), BF16),
        V((S, Dl), BF16), V((S, Dl), BF16),
        V((tokens, width), F32), V((tokens, width), F32), V((tokens, width), F32),
        V((tokens, width), BF16), V((tokens, width), F32),
        V((heads, HEAD_DIM, HEAD_DIM), F32), V((heads, 16, HEAD_DIM), F32),
        V((heads, HEAD_DIM, HEAD_DIM), F32), V((heads, 16, HEAD_DIM), F32),
        V((nhops, heads, HEAD_DIM + 16, HEAD_DIM), BF16),
        V((nhops, heads, HEAD_DIM + 16, HEAD_DIM), BF16),
        V((tokens, width), BF16), V((2, G, R, D), BF16), V((G, R, D), BF16),
        V((max(G - 1, 1), R, D), BF16), V((max(G - 1, 1), R, D), BF16),
        pltpu.SemaphoreType.DMA((4,)),
        pltpu.SemaphoreType.DMA((copies,)),
        pltpu.SemaphoreType.DMA((copies,)),
    ]
    return pl.pallas_call(
        functools.partial(kernel, E, T, cap, pieces),
        out_shape=(
            jax.ShapeDtypeStruct((R, D), BF16),
            jax.ShapeDtypeStruct((ntok, Dl), BF16),
        ),
        in_specs=[vm] * 7 + [anyspace] + [vm] * 4 + [anyspace] * 3,
        out_specs=(vm, vm),
        scratch_shapes=scratch,
        compiler_params=pltpu.CompilerParams(
            collective_id=0, has_side_effects=True, vmem_limit_bytes=60 * 1024 * 1024
        ),
    )(
        q, f, v, o, gap[None], extra, hscale[None], mixw, tok, escale[None],
        routes.T, scores.T, gate[0], up[0], down[0],
    )


def solution(mesh):
    E, T = mesh.shape["ep"], mesh.shape["tp"]
    return jax.shard_map(
        functools.partial(body, E, T),
        mesh=mesh,
        in_specs=(
            P("ep", "tp"),
            P("ep", "tp"),
            P("ep", "tp"),
            P("ep", "tp"),
            P("tp"),
            P("ep", "tp"),
            P("tp"),
            P("tp", None),
            P("ep", None),
            P(),
            P("ep", None),
            P("ep", None),
            P("ep", None, "tp"),
            P("ep", None, "tp"),
            P("ep", None, "tp"),
        ),
        out_specs=(P(("ep", "tp"), None), P("ep", "tp")),
        check_vma=False,
    )
```

```python
import functools

import jax
import jax.numpy as jnp
from jax import lax
from jax.experimental import pallas as pl
from jax.experimental.pallas import tpu as pltpu
from jax.sharding import PartitionSpec as P

HEAD_DIM = 128
CHUNK = 64
MESH = pl.DeviceIdType.MESH
F32 = jnp.float32
BF16 = jnp.bfloat16


def flip(i, k):
    b = 1
    while b <= k:
        if k & b:
            i = i + b - 2 * b * lax.rem(lax.div(i, b), 2)
        b *= 2
    return i


def kernel(
    E, T, cap, pieces,
    q_ref, f_ref, v_ref, o_ref, gap_ref, extra_ref, hscale_ref,
    mixw_hbm, tok_ref, escale_ref, routes_ref, scores_ref,
    gate_hbm, up_hbm, down_hbm,
    mix_out, exp_out,
    gate, up, down, mixw,
    ncols, dmat, wmat, outgoing, feats, hidden, part, precv, xsend, xrecv, fin, ret,
    qs, ks, run, qg, rec, ist, idec, est, edec, ksend, krecv,
    mhid, mpart, mprecv, mxsend, mxrecv,
    wsem, send_sem, recv_sem,
):
    me = lax.axis_index("ep")
    t = lax.axis_index("tp")
    G = T // 2
    g, c = lax.div(t, 2), lax.rem(t, 2)
    oc = 1 - c
    tokens, width = q_ref.shape
    heads = width // HEAD_DIM
    S = E * cap
    Dl = ncols.shape[1]
    FFl = hidden.shape[1]

    loads = [
        pltpu.make_async_copy(src, dst, wsem.at[i])
        for i, (src, dst) in enumerate(
            ((gate_hbm, gate), (up_hbm, up), (down_hbm, down), (mixw_hbm, mixw))
        )
    ]
    for load in loads:
        load.start()

    barrier = pltpu.get_barrier_semaphore()
    for k in range(1, E):
        pl.semaphore_signal(barrier, inc=1, device_id=(flip(me, k), t), device_id_type=MESH)
    pl.semaphore_signal(barrier, inc=1, device_id=(me, 2 * g + oc), device_id_type=MESH)
    for j in range(1, G):
        pl.semaphore_signal(
            barrier, inc=1, device_id=(me, 2 * flip(g, j) + c), device_id_type=MESH
        )

    used = [0]

    def remote(src, dst, device):
        slot = used[0]
        used[0] += 1
        return pltpu.make_async_remote_copy(
            src_ref=src, dst_ref=dst, send_sem=send_sem.at[slot], recv_sem=recv_sem.at[slot],
            device_id=device, device_id_type=MESH,
        )

    sent = []

    x = tok_ref[...].astype(F32)
    mean = jnp.mean(x, axis=-1, keepdims=True)
    centred = x - mean
    inv = lax.rsqrt(jnp.mean(centred * centred, axis=-1, keepdims=True) + 1e-05)
    cols = pl.ds(pl.multiple_of(t * Dl, 128), Dl)
    ncols[...] = ((tok_ref[:, cols].astype(F32) - mean) * inv * escale_ref[:, cols]).astype(BF16)

    ntok = tok_ref.shape[0]
    ek = lax.broadcasted_iota(jnp.int32, (E, ntok), 0) ^ me
    first, second = routes_ref[0:1, :] == ek, routes_ref[1:2, :] == ek
    named = jnp.where(first | second, 1.0, 0.0)
    earlier = jnp.where(
        lax.broadcasted_iota(jnp.int32, (ntok, ntok), 0)
        < lax.broadcasted_iota(jnp.int32, (ntok, ntok), 1), 1.0, 0.0
    ).astype(BF16)
    position = jnp.dot(named.astype(BF16), earlier, preferred_element_type=F32)
    place = jnp.where(first | second, position, -1.0).astype(jnp.int32)
    w0 = jax.nn.sigmoid(scores_ref[0:1, :] - scores_ref[1:2, :])
    weight = jnp.where(first, w0, jnp.where(second, 1.0 - w0, 0.0))
    rows = lax.broadcasted_iota(jnp.int32, (cap, ntok), 0)
    for k in range(E):
        hit = rows == place[k:k + 1, :]
        dmat[k * cap:(k + 1) * cap, :] = jnp.where(hit, 1.0, 0.0).astype(BF16)
        wmat[k * cap:(k + 1) * cap, :] = jnp.where(hit, weight[k:k + 1, :], 0.0).astype(BF16)
    outgoing[...] = jnp.dot(dmat[...], ncols[...], preferred_element_type=F32).astype(BF16)
    feats[t, 0:cap, :] = outgoing[0:cap, :]

    pl.semaphore_wait(barrier, E - 1 + 1 + G - 1)

    dispatch = {}
    for k in range(1, E):
        block = pl.ds(k * cap, cap)
        dispatch[k] = remote(outgoing.at[block], feats.at[t, block], (flip(me, k), t))
        dispatch[k].start()
        sent.append(dispatch[k])

    closing = gap_ref[...] * jax.nn.sigmoid(-f_ref[...].astype(F32))
    ks[...] = closing
    logd = jnp.log1p(-closing) + extra_ref[...]
    qs[...] = jax.nn.silu(q_ref[...].astype(F32))
    r_i = lax.broadcasted_iota(jnp.int32, (CHUNK, CHUNK), 0)
    c_i = lax.broadcasted_iota(jnp.int32, (CHUNK, CHUNK), 1)
    causal = r_i >= c_i
    tri = jnp.where(causal, 1.0, 0.0).astype(F32)
    nchunks = tokens // CHUNK
    for n in range(nchunks):
        run[n * CHUNK:(n + 1) * CHUNK, :] = jnp.dot(
            tri, logd[n * CHUNK:(n + 1) * CHUNK, :], precision=lax.Precision.HIGHEST,
            preferred_element_type=F32,
        )

    def head_local(h, _):
        lanes = pl.ds(pl.multiple_of(h * HEAD_DIM, HEAD_DIM), HEAD_DIM)
        state = jnp.zeros((HEAD_DIM, HEAD_DIM), F32)
        before = jnp.zeros((1, HEAD_DIM), F32)
        for n in range(nchunks):
            rs = slice(n * CHUNK, (n + 1) * CHUNK)
            r = run[rs, lanes]
            total = r[CHUNK - 1:CHUNK, :]
            qd = qs[rs, lanes] * jnp.exp(r)
            key = ks[rs, lanes]
            kd = (key * jnp.exp(-r)).astype(BF16)
            kst = (key * jnp.exp(total - r)).astype(BF16)
            val = v_ref[rs, lanes]
            qd_b = qd.astype(BF16)
            scores = lax.dot_general(
                qd_b, kd, (((1,), (1,)), ((), ())), preferred_element_type=F32
            )
            scores = jnp.where(causal, scores, 0.0).astype(BF16)
            out = jnp.dot(scores, val, preferred_element_type=F32)
            if n:
                out += lax.dot_general(
                    qd_b, state.astype(BF16), (((1,), (1,)), ((), ())),
                    preferred_element_type=F32,
                )
            rec[rs, lanes] = out
            qg[rs, lanes] = (qd * jnp.exp(before)).astype(BF16)
            state = state * jnp.exp(total) + lax.dot_general(
                val, kst, (((0,), (0,)), ((), ())), preferred_element_type=F32
            )
            before = before + total
        ist[h] = state
        idec[h] = jnp.broadcast_to(jnp.exp(before), (16, HEAD_DIM))
        est[h] = jnp.zeros((HEAD_DIM, HEAD_DIM), F32)
        edec[h] = jnp.ones((16, HEAD_DIM), F32)
        return 0

    lax.fori_loop(0, heads, head_local, 0)

    hops = []
    dist = 1
    while dist < E:
        hops.append(dist)
        dist *= 2
    hop_copy = [
        remote(ksend.at[r], krecv.at[r], (lax.rem(me + d, E), t)) for r, d in enumerate(hops)
    ]

    def hop_send(r):
        @pl.when(me + hops[r] < E)
        def _():
            ksend[r, :, 0:HEAD_DIM, :] = ist[...].astype(BF16)
            ksend[r, :, HEAD_DIM:HEAD_DIM + 16, :] = idec[...].astype(BF16)
            hop_copy[r].start()

    def hop_recv(r):
        @pl.when(me >= hops[r])
        def _():
            hop_copy[r].wait_recv()
            s = krecv[r, :, 0:HEAD_DIM, :].astype(F32)
            d = krecv[r, :, HEAD_DIM:HEAD_DIM + 16, :].astype(F32)
            est[...] = edec[:, 0:1, :] * s + est[...]
            edec[...] = edec[...] * d
            if r + 1 < len(hops):
                ist[...] = idec[:, 0:1, :] * s + ist[...]
                idec[...] = idec[...] * d

    hop_send(0)

    ag_partner, ag_cross, rs_partner, rs_cross, back = {}, {}, {}, {}, {}

    def piece_rows(p):
        a, n = pieces[p]
        return pl.ds(a * cap, n * cap)

    def gather_start(p):
        a, n = pieces[p]
        for k in range(max(a, 1), a + n):
            dispatch[k].wait_recv()
        rr = piece_rows(p)
        for j in range(1, G):
            ag_cross[p, j] = remote(feats.at[t, rr], feats.at[t, rr], (me, 2 * flip(g, j) + c))
            ag_cross[p, j].start()
            sent.append(ag_cross[p, j])
        for j in range(G):
            idx = 2 * flip(g, j) + c
            ag_partner[p, j] = (
                used[0], remote(feats.at[idx, rr], feats.at[idx, rr], (me, 2 * g + oc))
            )
        ag_partner[p, 0][1].start()
        sent.append(ag_partner[p, 0][1])

    def gather_relay(p):
        rr = piece_rows(p)
        for j in range(1, G):
            ag_cross[p, j].wait_recv()
            ag_partner[p, j][1].start()
            sent.append(ag_partner[p, j][1])

    def gather_end(p):
        for j in range(G):
            ag_partner[p, j][1].wait_recv()

    tile = min(256, FFl)

    def experts(p):
        a, n = pieces[p]
        rs = slice(a * cap, (a + n) * cap)

        def one(i, _):
            cc = pl.ds(pl.multiple_of(i * tile, tile), tile)
            ga = jnp.zeros((n * cap, tile), F32)
            ua = jnp.zeros((n * cap, tile), F32)
            for d in range(T):
                xs = feats[d, rs, :]
                ga += jnp.dot(xs, gate[d * Dl:(d + 1) * Dl, cc], preferred_element_type=F32)
                ua += jnp.dot(xs, up[d * Dl:(d + 1) * Dl, cc], preferred_element_type=F32)
            hidden[rs, cc] = (jax.nn.silu(ga) * ua).astype(BF16)
            return 0

        lax.fori_loop(0, FFl // tile, one, 0)

        def down_group(cls, gg):
            ff = pl.ds(pl.multiple_of((2 * gg + cls) * Dl, 128), Dl)
            part[cls, gg, rs, :] = lax.dot_general(
                hidden[rs, :], down[ff, :], (((1,), (1,)), ((), ())),
                preferred_element_type=F32,
            ).astype(BF16)

        def theirs(gg, _):
            down_group(oc, gg)
            return 0

        def ours(gg, _):
            down_group(c, gg)
            return 0

        lax.fori_loop(0, G, theirs, 0)
        rr = piece_rows(p)
        rs_partner[p] = remote(part.at[oc, :, rr], precv.at[:, rr], (me, 2 * g + oc))
        rs_partner[p].start()
        sent.append(rs_partner[p])
        lax.fori_loop(0, G, ours, 0)

    def scatter_cross(p):
        a, n = pieces[p]
        rs = slice(a * cap, (a + n) * cap)
        rr = piece_rows(p)
        rs_partner[p].wait_recv()
        for j in range(1, G):
            gj = flip(g, j)
            xsend[j - 1, rs, :] = (
                part[c, gj, rs, :].astype(F32) + precv[gj, rs, :].astype(F32)
            ).astype(BF16)
            rs_cross[p, j] = remote(
                xsend.at[j - 1, rr], xrecv.at[j - 1, rr], (me, 2 * gj + c)
            )
            rs_cross[p, j].start()
            sent.append(rs_cross[p, j])

    def give_back(p):
        a, n = pieces[p]
        rs = slice(a * cap, (a + n) * cap)
        total = part[c, g, rs, :].astype(F32) + precv[g, rs, :].astype(F32)
        for j in range(1, G):
            rs_cross[p, j].wait_recv()
            total += xrecv[j - 1, rs, :].astype(F32)
        fin[rs, :] = total.astype(BF16)
        for k in range(max(a, 1), a + n):
            block = pl.ds(k * cap, cap)
            back[k] = remote(fin.at[block], ret.at[block], (flip(me, k), t))
            back[k].start()
            sent.append(back[k])
        if a == 0:
            ret[0:cap, :] = fin[0:cap, :]

    def mixer_end():
        for load in loads[3:]:
            load.wait()
        for h in range(heads):
            lanes = slice(h * HEAD_DIM, (h + 1) * HEAD_DIM)
            r = rec[:, lanes] + lax.dot_general(
                qg[:, lanes], est[h].astype(BF16), (((1,), (1,)), ((), ())),
                preferred_element_type=F32,
            )
            r = r * lax.rsqrt(jnp.mean(r * r, axis=-1, keepdims=True) + 1e-06)
            mhid[:, lanes] = (
                r * hscale_ref[:, lanes] * jax.nn.silu(o_ref[:, lanes].astype(F32))
            ).astype(BF16)
        R = mix_out.shape[0]
        wide = mixw.shape[1]
        step = min(512, wide)

        def one(i, _):
            cc = pl.ds(pl.multiple_of(i * step, step), step)
            y = jnp.dot(mhid[...], mixw[:, cc], preferred_element_type=F32).astype(BF16)
            for d in range(T):
                mpart[d % 2, d // 2, :, cc] = y[d * R:(d + 1) * R, :]
            return 0

        lax.fori_loop(0, wide // step, one, 0)
        rs_partner["m"] = remote(mpart.at[oc], mprecv, (me, 2 * g + oc))
        rs_partner["m"].start()
        sent.append(rs_partner["m"])

    def mixer_cross():
        rs_partner["m"].wait_recv()
        for j in range(1, G):
            gj = flip(g, j)
            mxsend[j - 1] = (mpart[c, gj].astype(F32) + mprecv[gj].astype(F32)).astype(BF16)
            rs_cross["m", j] = remote(mxsend.at[j - 1], mxrecv.at[j - 1], (me, 2 * gj + c))
            rs_cross["m", j].start()
            sent.append(rs_cross["m", j])

    def mixer_out():
        total = mpart[c, g].astype(F32) + mprecv[g].astype(F32)
        for j in range(1, G):
            rs_cross["m", j].wait_recv()
            total += mxrecv[j - 1].astype(F32)
        mix_out[...] = total.astype(BF16)

    last = len(pieces) - 1
    hop_next = 1
    gather_start(0)
    hop_recv(0)
    if len(hops) > 1:
        hop_send(1)
    gather_relay(0)
    for load in loads[:3]:
        load.wait()
    for p in range(len(pieces)):
        if p < last:
            gather_start(p + 1)
        gather_end(p)
        if p > 0:
            scatter_cross(p - 1)
        experts(p)
        if p < last:
            gather_relay(p + 1)
        if p > 0:
            give_back(p - 1)
        if p + 2 < len(hops) and p < last:
            hop_recv(p + 1)
            hop_send(p + 2)
            hop_next = p + 2
    scatter_cross(last)
    for r in range(hop_next, len(hops)):
        hop_recv(r)
        if r + 1 < len(hops):
            hop_send(r + 1)
    mixer_end()
    give_back(last)
    mixer_cross()
    mixer_out()
    for k in range(1, E):
        back[k].wait_recv()
    exp_out[...] = lax.dot_general(
        wmat[...], ret[...], (((0,), (0,)), ((), ())), preferred_element_type=F32
    ).astype(BF16)
    for copy in sent:
        copy.wait_send()
    for r in range(len(hops)):
        @pl.when(me + hops[r] < E)
        def _():
            hop_copy[r].wait_send()


def body(E, T, q, f, v, o, gap, extra, hscale, mixw, tok, escale, routes, scores, gate, up, down):
    tokens, width = q.shape
    ntok, D = tok.shape
    heads = width // HEAD_DIM
    G = T // 2
    cap = -(-(3 * ntok // E) // 16) * 16
    S = E * cap
    Dl = D // T
    FFl = gate.shape[2]
    R = tokens // T
    half, quarter = E // 2, E // 4
    pieces = ((0, half), (half, quarter), (half + quarter, quarter))
    nhops = max(1, (E - 1).bit_length())
    copies = 2 * (E - 1) + nhops + len(pieces) * (G - 1 + G + 1 + G - 1) + G
    vm = pl.BlockSpec(memory_space=pltpu.VMEM)
    anyspace = pl.BlockSpec(memory_space=pl.ANY)
    V = pltpu.VMEM
    scratch = [
        V((D, FFl), BF16), V((D, FFl), BF16), V((D, FFl), BF16), V(mixw.shape, BF16),
        V((ntok, Dl), BF16), V((S, ntok), BF16), V((S, ntok), BF16), V((S, Dl), BF16),
        V((T, S, Dl), BF16), V((S, FFl), BF16), V((2, G, S, Dl), BF16), V((G, S, Dl), BF16),
        V((max(G - 1, 1), S, Dl), BF16), V((max(G - 1, 1), S, Dl), BF16),
        V((S, Dl), BF16), V((S, Dl), BF16),
        V((tokens, width), F32), V((tokens, width), F32), V((tokens, width), F32),
        V((tokens, width), BF16), V((tokens, width), F32),
        V((heads, HEAD_DIM, HEAD_DIM), F32), V((heads, 16, HEAD_DIM), F32),
        V((heads, HEAD_DIM, HEAD_DIM), F32), V((heads, 16, HEAD_DIM), F32),
        V((nhops, heads, HEAD_DIM + 16, HEAD_DIM), BF16),
        V((nhops, heads, HEAD_DIM + 16, HEAD_DIM), BF16),
        V((tokens, width), BF16), V((2, G, R, D), BF16), V((G, R, D), BF16),
        V((max(G - 1, 1), R, D), BF16), V((max(G - 1, 1), R, D), BF16),
        pltpu.SemaphoreType.DMA((4,)),
        pltpu.SemaphoreType.DMA((copies,)),
        pltpu.SemaphoreType.DMA((copies,)),
    ]
    return pl.pallas_call(
        functools.partial(kernel, E, T, cap, pieces),
        out_shape=(
            jax.ShapeDtypeStruct((R, D), BF16),
            jax.ShapeDtypeStruct((ntok, Dl), BF16),
        ),
        in_specs=[vm] * 7 + [anyspace] + [vm] * 4 + [anyspace] * 3,
        out_specs=(vm, vm),
        scratch_shapes=scratch,
        compiler_params=pltpu.CompilerParams(
            collective_id=0, has_side_effects=True, vmem_limit_bytes=60 * 1024 * 1024
        ),
    )(
        q, f, v, o, gap[None], extra, hscale[None], mixw, tok, escale[None],
        routes.T, scores.T, gate[0], up[0], down[0],
    )


def solution(mesh):
    E, T = mesh.shape["ep"], mesh.shape["tp"]
    return jax.shard_map(
        functools.partial(body, E, T),
        mesh=mesh,
        in_specs=(
            P("ep", "tp"),
            P("ep", "tp"),
            P("ep", "tp"),
            P("ep", "tp"),
            P("tp"),
            P("ep", "tp"),
            P("tp"),
            P("tp", None),
            P("ep", None),
            P(),
            P("ep", None),
            P("ep", None),
            P("ep", None, "tp"),
            P("ep", None, "tp"),
            P("ep", None, "tp"),
        ),
        out_specs=(P(("ep", "tp"), None), P("ep", "tp")),
        check_vma=False,
    )
```
